512 devices in a mesh: sp: 128 (over z, y, core), tp: 4 (over x).
Axes of the slice: x: 4, y: 8, z: 8, core: 2. Of those that a mesh axis runs over, the one named last changes fastest.
Arguments:
- tokens: bfloat16 [16384, 2048], P(('sp', 'tp')), may hold values from -8.5 to 8.5
- norm_gain: bfloat16 [2048], replicated, may hold values from 0.099609375 to 1.8984375
- w_query: bfloat16 [2048, 1024], P(None, 'tp'), may hold values from -0.088388348 to 0.088388348
- w_key: bfloat16 [2048, 512], P(None, 'tp'), may hold values from -5.3298174 to 5.3298174
- w_value: bfloat16 [2048, 512], P(None, 'tp'), may hold values from -0.125 to 0.125
- w_conv_value: bfloat16 [2048, 1024], P(None, 'tp'), may hold values from -0.125 to 0.125
- w_conv_gate: bfloat16 [2048, 1024], P(None, 'tp'), may hold values from -0.125 to 0.125
- conv_taps: bfloat16 [31, 1024], P(None, 'tp'), may hold values from -1 to 1
- conv_gain: bfloat16 [1024], P('tp'), may hold values from 0.099609375 to 1.8984375
- conv_bias: bfloat16 [1024], P('tp'), may hold values from -3 to 3
- cum_gate: float32 [16384, 8], P(None, 'tp'), may hold values from -1969 to 0, as said below
- w_out_att: bfloat16 [1024, 2048], P('tp', 'sp'), may hold values from -0.28125 to 0.28125
- w_out_conv: bfloat16 [1024, 2048], P('tp', 'sp'), may hold values from -0.1875 to 0.1875
Outputs:
- mixed_out: bfloat16 [16384, 2048], P('sp', 'tp')
The draws below stay inside these ranges and needn't reach their ends.
Inputs may be any that keep to these rules, and one draw needn't show every extreme that they name: `cum_gate`: in each head, non-increasing along positions, and at most 0.
All inputs are finite; a program needn't handle non-finite values.
Results may differ from the reference program's by a relative error of at most 0.012.
Values may be sent and summed in bfloat16 or wider, within the bound.
A program may use at most 64 MiB of HBM per device.

```python
import math
import jax
import jax.numpy as jnp
from jax import lax

D = 2048
ASKER_HEAD_TALLY = 8
KV_HEADS = 4
HEAD = 128
CONV = 1024
KW = 31
TOK_DEV = 128
SERIES_ENTRIES = 16384


def draw_tokens(key, part):
    starting_number = jax.random.fold_in(key, 37)
    noise_key, direction_key, orientation_key = jax.random.split(starting_number, 3)
    noise = jax.random.truncated_normal(noise_key, -4.0, 4.0, (SERIES_ENTRIES, D), jnp.float32)
    direction = jax.random.truncated_normal(direction_key, -3.0, 3.0, (D,), jnp.float32)
    orientation = jnp.where(jax.random.bernoulli(orientation_key), 1.0, -1.0)
    places = jnp.arange(SERIES_ENTRIES, dtype=jnp.float32)
    drift_line = 1.5 * orientation * (2.0 * places / (SERIES_ENTRIES - 1) - 1.0)
    return (noise + drift_line[:, None] * direction[None, :]).astype(jnp.bfloat16)


def query_key_pair(key):
    starting_number = jax.random.fold_in(key, 11)
    first_key = jax.random.fold_in(starting_number, 0)
    second_key = jax.random.fold_in(starting_number, 1)
    mixing_key = jax.random.fold_in(starting_number, 3)
    scale = D ** (-0.5)
    weight_query = jax.random.truncated_normal(first_key, -4.0, 4.0, (D, ASKER_HEAD_TALLY * HEAD), jnp.float32) * scale
    weight_key = jax.random.truncated_normal(second_key, -4.0, 4.0, (D, KV_HEADS * HEAD), jnp.float32) * scale
    grouped = weight_query.reshape(D, KV_HEADS, ASKER_HEAD_TALLY // KV_HEADS, HEAD).sum(axis=2).reshape(D, KV_HEADS * HEAD)
    mixing = jax.random.uniform(mixing_key, (KV_HEADS,), jnp.float32, -0.7, -0.4)
    mixing_columns = jnp.repeat(mixing, HEAD)
    mixed = grouped * mixing_columns[None, :] + weight_key
    weight_key = mixed
    return (weight_query, weight_key)


def draw_w_query(key, part):
    return query_key_pair(key)[0].astype(jnp.bfloat16)


def draw_w_key(key, part):
    return query_key_pair(key)[1].astype(jnp.bfloat16)


def draw_cum_gate(key, part):
    starting_number = jax.random.fold_in(key, 23)
    shuffle_seed_handle, quick_seed_handle, gradual_seed_handle, tile_seed_handle, coarse_seed_handle, spurt_seed_handle, channelwise_seed_handle = jax.random.split(starting_number, 7)
    ranks = jnp.argsort(jax.random.permutation(shuffle_seed_handle, ASKER_HEAD_TALLY))
    fast_heads = ranks < ASKER_HEAD_TALLY // 2
    fast_rate = jnp.exp(jax.random.uniform(quick_seed_handle, (ASKER_HEAD_TALLY,), jnp.float32, math.log(1.0 / 100.0), math.log(1.0 / 30.0)))
    slow_total = jax.random.uniform(gradual_seed_handle, (ASKER_HEAD_TALLY,), jnp.float32, 0.2, 0.4)
    rate = jnp.where(fast_heads, fast_rate, slow_total / SERIES_ENTRIES)
    block_factor = jnp.exp(jax.random.uniform(tile_seed_handle, (SERIES_ENTRIES // TOK_DEV, ASKER_HEAD_TALLY), jnp.float32, math.log(0.5), math.log(2.0)))
    block_factor = jnp.repeat(block_factor, TOK_DEV, axis=0)
    rough = jax.random.uniform(coarse_seed_handle, (SERIES_ENTRIES, ASKER_HEAD_TALLY), jnp.float32, 0.2, 1.8)
    iteration_tally = -rate[None, :] * block_factor * rough
    spot_number = jax.random.randint(spurt_seed_handle, (2, ASKER_HEAD_TALLY), 0, SERIES_ENTRIES)
    objective_number = jax.random.uniform(channelwise_seed_handle, (2, ASKER_HEAD_TALLY), jnp.float32, 0.2, 0.35)
    location_number = jnp.arange(SERIES_ENTRIES, dtype=jnp.int32)
    for spurt_extent in range(2):
        match_selector = location_number[:, None] == spot_number[spurt_extent][None, :]
        iteration_tally = iteration_tally + jnp.where(match_selector, jnp.log(1.0 - objective_number[spurt_extent])[None, :], 0.0)
    return jnp.cumsum(iteration_tally, axis=0).astype(jnp.float32)


def block_levels(own_key, shape, cuts, low, largest):
    factor_of, own = 1.0, jax.random.fold_in(own_key, 6)
    for dim, shards_of in cuts:
        draws = jnp.exp(jax.random.uniform(jax.random.fold_in(own, dim), (shards_of,), jnp.float32, low / len(cuts), largest / len(cuts)))
        factor_of = factor_of * jnp.repeat(draws, shape[dim] // shards_of).reshape([-1 if axis == dim else 1 for axis in range(len(shape))])
    return factor_of


def centred(key, shape, deviation, limit, shards=(), held_as=jnp.bfloat16):
    entries = deviation * jax.random.normal(key, shape, jnp.float32)
    if shards:
        entries = entries * block_levels(key, shape, shards, -0.22, 0.18)
    return jnp.clip(entries, -limit, limit).astype(held_as)


def setup_inputs(seed: int = 0) -> dict:
    key_of = jax.random.split(jax.random.key(seed), 14)
    return {
        "tokens": draw_tokens(jax.random.fold_in(key_of[13], 71), 0),
        "norm_gain": jnp.clip(1.0 + 0.18 * jax.random.normal(key_of[1], (D,), jnp.float32), 0.099609375, 1.8984375).astype(jnp.bfloat16),
        "w_query": draw_w_query(jax.random.fold_in(key_of[13], 71), 0),
        "w_key": draw_w_key(jax.random.fold_in(key_of[13], 71), 0),
        "w_value": centred(key_of[4], (D, KV_HEADS * HEAD), D ** -0.5, 0.125, ((1, 4),)),
        "w_conv_value": centred(key_of[5], (D, CONV), D ** -0.5, 0.125, ((1, 4),)),
        "w_conv_gate": centred(key_of[6], (D, CONV), D ** -0.5, 0.125, ((1, 4),)),
        "conv_taps": centred(key_of[7], (KW, CONV), KW ** -0.5, 1.0, ((1, 4),)),
        "conv_gain": jnp.clip(1.0 + 0.18 * jax.random.normal(key_of[8], (CONV,), jnp.float32), 0.099609375, 1.8984375).astype(jnp.bfloat16),
        "conv_bias": centred(key_of[9], (CONV,), 0.5, 3.0, ((0, 4),)),
        "cum_gate": draw_cum_gate(jax.random.fold_in(key_of[13], 71), 0),
        "w_out_att": centred(key_of[11], (ASKER_HEAD_TALLY * HEAD, D), (1.5 / (ASKER_HEAD_TALLY * HEAD) ** 0.5), 0.28125, ((0, 4), (1, 128))),
        "w_out_conv": centred(key_of[12], (CONV, D), CONV ** -0.5, 0.1875, ((0, 4), (1, 128))),
    }


def reference(tokens, norm_gain, w_query, w_key, w_value, w_conv_value, w_conv_gate, conv_taps, conv_gain, conv_bias, cum_gate, w_out_att, w_out_conv):
    floats = tokens.astype(jnp.float32)
    normed = (floats * lax.rsqrt(lax.optimization_barrier(jnp.mean(floats * floats, axis=-1, keepdims=True)) + 1e-06) * norm_gain.astype(jnp.float32)).astype(jnp.bfloat16)
    query = jnp.dot(normed, w_query, preferred_element_type=jnp.float32).astype(jnp.bfloat16)
    key_rows = jnp.dot(normed, w_key, preferred_element_type=jnp.float32).astype(jnp.bfloat16)
    value_rows = jnp.dot(normed, w_value, preferred_element_type=jnp.float32).astype(jnp.bfloat16)
    group_size = ASKER_HEAD_TALLY // KV_HEADS
    query_heads = query.astype(jnp.float32).reshape(SERIES_ENTRIES, ASKER_HEAD_TALLY, HEAD)
    key_heads = jnp.repeat(key_rows.astype(jnp.float32).reshape(SERIES_ENTRIES, KV_HEADS, HEAD), group_size, axis=1)
    value_heads = jnp.repeat(value_rows.astype(jnp.float32).reshape(SERIES_ENTRIES, KV_HEADS, HEAD), group_size, axis=1)
    block_rows = math.gcd(SERIES_ENTRIES, 256)
    scale = 1.0 / math.sqrt(HEAD)
    gates_by_head = cum_gate.T
    key_places = jnp.arange(SERIES_ENTRIES, dtype=jnp.int32)

    def one_block(index):
        first = (index * block_rows).astype(jnp.int32)
        query_block = lax.dynamic_slice_in_dim(query_heads, first, block_rows, 0)
        gate_block = lax.dynamic_slice_in_dim(cum_gate, first, block_rows, 0)
        scores = jnp.einsum('thd,shd->hts', query_block, key_heads) * scale
        logits = scores + gate_block.T[:, :, None] - gates_by_head[:, None, :]
        query_places = first + jnp.arange(block_rows, dtype=jnp.int32)
        allowed = key_places[None, :] <= query_places[:, None]
        logits = jnp.where(allowed[None], logits, -jnp.inf)
        row_max = lax.optimization_barrier(jnp.max(logits, axis=-1, keepdims=True))
        weights = jnp.where(allowed[None], jnp.exp(logits - row_max), 0.0)
        denom = lax.optimization_barrier(jnp.sum(weights, axis=-1))
        rounded = lax.optimization_barrier(weights.astype(jnp.bfloat16)).astype(jnp.float32)
        numer = jnp.einsum('hts,shd->htd', rounded, value_heads)
        return (numer / denom[:, :, None]).astype(jnp.bfloat16)
    blocks = lax.map(one_block, jnp.arange(SERIES_ENTRIES // block_rows, dtype=jnp.int32))
    attended = jnp.transpose(blocks, (0, 2, 1, 3)).reshape(SERIES_ENTRIES, ASKER_HEAD_TALLY * HEAD)
    value_part = jnp.dot(normed, w_conv_value, preferred_element_type=jnp.float32)
    gate_part = jnp.dot(normed, w_conv_gate, preferred_element_type=jnp.float32)
    glu = (value_part * jax.nn.sigmoid(gate_part)).astype(jnp.bfloat16)
    padded = jnp.concatenate([jnp.zeros((KW - 1, CONV), jnp.bfloat16), glu], axis=0).astype(jnp.float32)
    taps = conv_taps.astype(jnp.float32)
    conv = jnp.zeros((SERIES_ENTRIES, CONV), jnp.float32)
    for shift_tap in range(KW):
        conv = conv + taps[shift_tap][None, :] * padded[shift_tap:shift_tap + SERIES_ENTRIES]
    mean_c = lax.optimization_barrier(jnp.mean(conv, axis=-1, keepdims=True))
    var_c = lax.optimization_barrier(jnp.mean(conv * conv, axis=-1, keepdims=True)) - mean_c * mean_c
    shaped = (conv - mean_c) * lax.rsqrt(var_c + 1e-05) * conv_gain.astype(jnp.float32) + conv_bias.astype(jnp.float32)
    conv_act = jax.nn.silu(shaped).astype(jnp.bfloat16)
    total = jnp.dot(attended, w_out_att, preferred_element_type=jnp.float32) + jnp.dot(conv_act, w_out_conv, preferred_element_type=jnp.float32)
    return total.astype(jnp.bfloat16)
```

```python
import math

import jax
import jax.numpy as jnp
from jax import lax
from jax.experimental import pallas as pl
from jax.experimental.pallas import tpu as pltpu
from jax.sharding import PartitionSpec as P

HEAD = 128
KW = 31
ROWS = 128
LOG2E = math.log2(math.e)
FAR = 1e30
MESH = pl.DeviceIdType.MESH
F32 = jnp.float32
BF16 = jnp.bfloat16


def nt(a, b):
    return lax.dot_general(a, b, (((1,), (1,)), ((), ())), preferred_element_type=F32)


def nn(a, b):
    return lax.dot_general(a, b, (((1,), (0,)), ((), ())), preferred_element_type=F32)


class Sems:
    def __init__(self, send, recv):
        self.send, self.recv, self.used = send, recv, 0

    def take(self, count=1):
        first = self.used
        self.used += count
        return first


class Ring:
    def __init__(self, n, sems, chunks, plus, minus, here, there):
        self.n, self.chunks, self.here, self.there = n, chunks, here, there
        self.peer = {1: plus, -1: minus}
        self.hops = {1: n // 2, -1: (n - 1) // 2}
        self.base = sems.take((n - 1) * chunks) if n > 1 else 0
        self.sems = sems
        self.started = []

    def index(self, way, k, ch):
        return self.base + ((k - 1) if way > 0 else self.hops[1] + k - 1) * self.chunks + ch

    def rel(self, way, k):
        return k if way > 0 else (self.n - k) % self.n

    def copy(self, way, k, ch):
        i = self.index(way, k, ch)
        a, b = self.rel(way, k - 1), self.rel(way, k)
        return pltpu.make_async_remote_copy(
            src_ref=self.here(a, ch),
            dst_ref=self.there(a, b, ch),
            send_sem=self.sems.send.at[i],
            recv_sem=self.sems.recv.at[i],
            device_id=self.peer[way],
            device_id_type=MESH,
        )

    def start(self, way, k, ch):
        if k <= self.hops[way]:
            c = self.copy(way, k, ch)
            c.start()
            self.started.append(c)

    def arrive(self, way, k, ch):
        i = self.index(way, k, ch)
        slot = self.here(self.rel(way, k), ch)
        pltpu.make_async_remote_copy(
            src_ref=slot,
            dst_ref=slot,
            send_sem=self.sems.send.at[i],
            recv_sem=self.sems.recv.at[i],
            device_id=self.peer[-way],
            device_id_type=MESH,
        ).wait_recv()

    def step(self, way, k, after=None):
        if k > self.hops[way]:
            return
        for ch in range(self.chunks):
            self.arrive(way, k, ch)
            self.start(way, k + 1, ch)
            if after is not None:
                after(self.rel(way, k), ch)


def layer_kernel(
    nz, ny, nx,
    tokens, gain, wq, wk, wv, wcv, wcg, taps, cgain, cbias, gate, wa_t, wc_t,
    out,
    tok_all, wbuf, qsend, qbuf, kv, conv_in, halo_out, halo_in, conv_s, st_out, st_in,
    wt, s_ref, gkb, o_out, o_in, rs_out, rs_in, proj_s, wsem, send, recv,
):
    rows = ROWS
    chip = 2 * rows
    dim = tokens.shape[1]
    trows = tokens.shape[0]
    chans = wcv.shape[1]
    ocols = out.shape[1]
    sp = lax.axis_index("sp")
    x = lax.axis_index("tp")
    c = lax.rem(sp, 2)
    y = lax.rem(lax.div(sp, 2), ny)
    z = lax.div(sp, 2 * ny)
    nsp = nz * ny * 2

    def at(zz, yy, cc):
        return (zz * ny + yy) * 2 + cc

    def mod(a, n):
        return lax.rem(a + 2 * n, n)

    sems = Sems(send, recv)
    pending = []

    def remote(src, dst, i, dev, ri=None):
        return pltpu.make_async_remote_copy(
            src_ref=src,
            dst_ref=dst,
            send_sem=send.at[i],
            recv_sem=recv.at[i if ri is None else ri],
            device_id=dev,
            device_id_type=MESH,
        )

    def launch(src, dst, i, dev, ri=None):
        cp = remote(src, dst, i, dev, ri)
        cp.start()
        pending.append(cp)

    sib = (at(z, y, 1 - c), x)

    wcols, off = [], 0
    for k, w in enumerate((wq, wk, wv, wcv, wcg)):
        cp = pltpu.make_async_copy(w, wbuf.at[:, off : off + w.shape[1]], wsem.at[k])
        cp.start()
        wcols.append(cp)
        off += w.shape[1]

    barrier = pltpu.get_barrier_semaphore()
    peers = [(sp, mod(x + d, nx)) for d in range(1, nx)]
    peers += [(at(z, mod(y + d, ny), cc), x) for d in range(1, ny) for cc in range(2)]
    peers += [sib]
    if nz > 1:
        peers += [(at(mod(z + d, nz), y, c), x) for d in (1, -1)]
    nxt, prv = mod(sp + 1, nsp), mod(sp - 1, nsp)
    peers += [(nxt, x), (prv, x)]
    for p in peers:
        pl.semaphore_signal(barrier, inc=1, device_id=p, device_id_type=MESH)

    tok = tokens[...].astype(F32)
    mean_sq = jnp.mean(tok * tok, axis=-1, keepdims=True)
    tok_all[x] = (tok * lax.rsqrt(mean_sq + 1e-06) * gain[...].astype(F32)).astype(BF16)
    wt[z, y, c, :, :256] = wa_t[...]
    wt[z, y, c, :, 256:] = wc_t[...]

    pl.semaphore_wait(barrier, len(peers))

    tok_i = sems.take(nx)
    order = sorted(range(1, nx), key=lambda d: -min(d, nx - d))
    for d in order:
        launch(tok_all.at[x], tok_all.at[x], tok_i + d, (sp, mod(x + d, nx)))

    wy = Ring(
        ny, sems, 1,
        (at(z, mod(y + 1, ny), c), x), (at(z, mod(y - 1, ny), c), x),
        lambda r, ch: wt.at[z, mod(y - r, ny), c],
        lambda a, b, ch: wt.at[z, mod(y - a, ny), c],
    )
    wz = Ring(
        nz, sems, 1,
        (at(mod(z + 1, nz), y, c), x), (at(mod(z - 1, nz), y, c), x),
        lambda r, ch: wt.at[mod(z - r, nz), :, c],
        lambda a, b, ch: wt.at[mod(z - a, nz), :, c],
    )
    qr = Ring(
        ny, sems, 2,
        (at(z, mod(y + 1, ny), c), x), (at(z, mod(y - 1, ny), c), x),
        lambda r, ch: qbuf.at[r, pl.ds(pl.multiple_of((c if ch == 0 else 1 - c) * rows, rows), rows)],
        lambda a, b, ch: qbuf.at[b, pl.ds(pl.multiple_of((c if ch == 0 else 1 - c) * rows, rows), rows)],
    )
    kr = Ring(
        nz, sems, 1,
        (at(mod(z + 1, nz), y, c), x), (at(mod(z - 1, nz), y, c), x),
        lambda r, ch: kv.at[r, 0],
        lambda a, b, ch: kv.at[b, 0],
    )
    for way in (1, -1):
        wy.start(way, 1, 0)

    g_first = gate[:, pl.ds(pl.multiple_of(z * ny * chip, chip), 128)]
    g_ref = jnp.where(c == 0, g_first[0:1, 0:1], g_first[1:2, 0:1])

    def gate_row(start, width):
        g = gate[:, pl.ds(pl.multiple_of(start, 128), width)]
        return (jnp.where(c == 0, g[0:1], g[1:2]) - g_ref) * LOG2E

    for s in range(nz):
        for p in range(2):
            cc = c if p == 0 else 1 - c
            g = gate_row(at(mod(z - s, nz), y, cc) * rows, rows)
            g = jnp.where(s <= z, g, FAR)
            gkb[pl.ds((s * 2 + p) * rows, rows), :] = jnp.transpose(jnp.broadcast_to(g, (128, rows)))

    for way in (1, -1):
        wy.step(way, 1)
        wy.step(way, 2)

    for cp in wcols[:3]:
        cp.wait()
    for d in range(1, nx):
        src = mod(x - d, nx)
        remote(tok_all.at[src], tok_all.at[src], tok_i + d, (sp, src)).wait_recv()
    normed = tok_all[...].reshape(rows, dim)
    qw, kw_ = wq.shape[1], wk.shape[1]
    qkv = nn(normed, wbuf[:, : qw + 2 * kw_])
    q0 = qkv[:, :HEAD].astype(BF16)
    q1 = qkv[:, HEAD:qw].astype(BF16)
    kv[0, 0, :rows] = qkv[:, qw : qw + kw_].astype(BF16)
    kv[0, 0, rows:] = jnp.transpose(qkv[:, qw + kw_ :]).astype(BF16)
    mine = pl.ds(pl.multiple_of(c * rows, rows), rows)
    qbuf[0, mine] = jnp.where(c == 0, q0, q1)
    qsend[...] = jnp.where(c == 0, q1, q0)

    q_i = sems.take()
    launch(qsend, qbuf.at[0, mine], q_i, sib)
    for way in (1, -1):
        qr.start(way, 1, 0)
        kr.start(way, 1, 0)
    ks_i = sems.take(nz)

    def pass_kv(rel, ch):
        launch(kv.at[rel, 0], kv.at[rel, 1], ks_i + rel, sib)

    pass_kv(0, 0)
    theirs = pl.ds(pl.multiple_of((1 - c) * rows, rows), rows)
    remote(qsend, qbuf.at[0, theirs], q_i, sib).wait_recv()
    for way in (1, -1):
        qr.start(way, 1, 1)

    for cp in wcols[3:]:
        cp.wait()
    halves = nn(normed, wbuf[:, qw + 2 * kw_ :])
    glu = (halves[:, :chans] * jax.nn.sigmoid(halves[:, chans:])).astype(BF16)
    conv_in[32:] = glu.astype(F32)
    halo_out[...] = glu[rows - 32 :]
    h_i = sems.take()
    launch(halo_out, halo_in, h_i, (nxt, x))

    for way in (1, -1):
        wy.step(way, 3)
        qr.step(way, 1)
        kr.step(way, 1, pass_kv)

    remote(halo_out, halo_in, h_i, (prv, x)).wait_recv()
    conv_in[:32] = jnp.where(sp == 0, 0.0, halo_in[...].astype(F32))

    for way in (1, -1):
        wy.step(way, 4)
        qr.step(way, 2)
        kr.step(way, 2, pass_kv)

    tap = taps[...].astype(F32)
    half = KW // 2
    conv = jnp.zeros((rows, chans), F32)
    for k in range(half):
        conv = conv + tap[k : k + 1] * conv_in[2 + k : 2 + k + rows]
    for way in (1, -1):
        qr.step(way, 3)
        kr.step(way, 3, pass_kv)
    for k in range(half, KW):
        conv = conv + tap[k : k + 1] * conv_in[2 + k : 2 + k + rows]
    conv_s[...] = conv
    s1 = jnp.sum(conv, axis=1, keepdims=True)
    s2 = jnp.sum(conv * conv, axis=1, keepdims=True)
    lane = lax.broadcasted_iota(jnp.int32, (rows, 128), 1)
    st_out[...] = jnp.transpose(jnp.where(lane == 0, s1, s2))[:8]
    st_i = sems.take(nx)
    for d in order:
        launch(st_out, st_in.at[nx - d], st_i + d, (sp, mod(x + d, nx)))
    for k in range(4, max([0] + [r.hops[1] for r in (qr, kr)]) + 1):
        for way in (1, -1):
            qr.step(way, k)
            kr.step(way, k, pass_kv)
    for way in (1, -1):
        wz.start(way, 1, 0)
    for s in range(nz):
        remote(kv.at[s, 0], kv.at[s, 1], ks_i + s, sib).wait_recv()

    scale = LOG2E / math.sqrt(HEAD)
    ones = jnp.ones((16, chip), BF16)
    o_i = sems.take(ny * 2)
    sub = lax.broadcasted_iota(jnp.int32, (16, rows), 0)
    key_lo = lax.broadcasted_iota(jnp.int32, (rows, chip), 0)
    q_at = lax.broadcasted_iota(jnp.int32, (rows, chip), 1)

    def attend(r):
        jq = mod(y - r, ny)
        qb = qbuf[r]
        peak = jnp.full((8, chip), -FAR, F32)
        for s in range(nz):
            for p in range(2):
                keys = kv[s, p, :rows]
                g = gkb[pl.ds((s * 2 + p) * rows, rows), :]
                t = nt(keys, qb) * scale - jnp.concatenate([g, g], axis=1)
                if s == 0:
                    cc = c if p == 0 else 1 - c
                    shift = (y - jq) * chip + cc * rows
                    t = jnp.where(key_lo + shift <= q_at, t, -FAR)
                s_ref[pl.ds((s * 2 + p) * rows, rows), :] = t
                peak = jnp.maximum(peak, jnp.max(t.reshape(rows // 8, 8, chip), axis=0))
        m = jnp.max(peak, axis=0, keepdims=True)
        acc = jnp.zeros((HEAD + 16, chip), F32)
        for s in range(nz):
            w = jnp.exp2(s_ref[pl.ds(s * chip, chip), :] - m).astype(BF16)
            vt = jnp.concatenate([kv[s, 0, rows:], kv[s, 1, rows:]], axis=1)
            acc = acc + nn(jnp.concatenate([vt, ones], axis=0), w)
        den = acc[HEAD : HEAD + 1]
        o = (acc[:HEAD] / den).astype(BF16)
        m = m + gate_row((z * ny + jq) * chip, chip)
        m1 = m.astype(BF16).astype(F32)
        m2 = (m - m1).astype(BF16).astype(F32)
        d1 = den.astype(BF16).astype(F32)
        d2 = (den - d1).astype(BF16).astype(F32)
        parts = (m1, m2, m - m1 - m2, d1, d2, den - d1 - d2)
        for cc in range(2):
            lanes = slice(cc * rows, (cc + 1) * rows)
            tile = jnp.zeros((16, rows), F32)
            for i, part in enumerate(parts):
                tile = jnp.where(sub == i, part[:, lanes], tile)
            o_out[r, cc, :HEAD] = o[:, lanes]
            o_out[r, cc, HEAD:] = tile.astype(BF16)

    ring_order = sorted(range(ny), key=lambda r: (-min(r, ny - r), r))
    for n, r in enumerate(ring_order):
        attend(r)
        if r:
            for cc in range(2):
                launch(o_out.at[r, cc], o_in.at[r, c], o_i + 2 * r + cc, (at(z, mod(y - r, ny), cc), x), o_i + 2 * r + c)
        if n % 2 == 1 and n // 2 + 1 <= nz // 2:
            for way in (1, -1):
                wz.step(way, n // 2 + 1)
    for k in range(ny // 2 + 1, nz // 2 + 1):
        for way in (1, -1):
            wz.step(way, k)
    launch(o_out.at[0, 1 - c], o_in.at[0, c], o_i + 1 - c, sib, o_i + c)

    ws_i = sems.take(nz)
    for s in range(nz):
        zz = mod(z - s, nz)
        launch(wt.at[zz, :, c], wt.at[zz, :, c], ws_i + s, sib)

    tot = st_out[...]
    for d in range(1, nx):
        remote(st_out, st_in.at[nx - d], st_i + d, (sp, mod(x - d, nx))).wait_recv()
        tot = tot + st_in[nx - d]
    total_chans = chans * nx
    mean_r = tot[0:1] / total_chans
    var_r = tot[1:2] / total_chans - mean_r * mean_r
    rstd_r = lax.rsqrt(var_r + 1e-05)
    mean_c = jnp.transpose(jnp.broadcast_to(mean_r, (128, rows)))
    rstd_c = jnp.transpose(jnp.broadcast_to(rstd_r, (128, rows)))
    wide = chans // 128
    mean_c = jnp.concatenate([mean_c] * wide, axis=1)
    rstd_c = jnp.concatenate([rstd_c] * wide, axis=1)
    shaped = (conv_s[...] - mean_c) * rstd_c * cgain[...].astype(F32) + cbias[...].astype(F32)
    conv_act = (shaped / (1.0 + jnp.exp(-shaped))).astype(BF16)

    for s in range(nz):
        zz = mod(z - s, nz)
        remote(wt.at[zz, :, 1 - c], wt.at[zz, :, 1 - c], ws_i + s, sib).wait_recv()
    per = nz // nx
    for d in range(nx):
        xx = mod(x + d, nx)
        w = wt[pl.ds(xx * per, per), :, :, :, 256:].reshape(ocols, chans)
        proj_s[d] = nt(conv_act, w)

    o_in[0, c] = o_out[0, c]
    for r in range(ny):
        for hh in range(2):
            if r:
                slot, frm = o_in.at[r, hh], (at(z, mod(y + r, ny), hh), x)
                remote(slot, slot, o_i + 2 * r + hh, frm).wait_recv()
    slot = o_in.at[0, 1 - c]
    remote(slot, slot, o_i + 1 - c, sib).wait_recv()
    heads = []
    for hh in range(2):
        tiles = [o_in[r, hh, HEAD:].astype(F32) for r in range(ny)]
        tops = [t[0:1] + t[1:2] + t[2:3] for t in tiles]
        dens = [t[3:4] + t[4:5] + t[5:6] for t in tiles]
        top = tops[0]
        for t in tops[1:]:
            top = jnp.maximum(top, t)
        scaled = [d * jnp.exp2(t - top) for d, t in zip(dens, tops)]
        den = scaled[0]
        for d in scaled[1:]:
            den = den + d
        acc = jnp.zeros((HEAD, rows), F32)
        for r in range(ny):
            acc = acc + o_in[r, hh, :HEAD].astype(F32) * (scaled[r] / den)
        heads.append(jnp.transpose(acc).astype(BF16))
    attended = jnp.concatenate(heads, axis=1)

    rs_i = sems.take(nx)
    for d in order + [0]:
        xx = mod(x + d, nx)
        w = wt[pl.ds(xx * per, per), :, :, :, :256].reshape(ocols, 256)
        part = proj_s[d] + nt(attended, w)
        if d:
            rs_out[d] = part.astype(BF16)
            launch(rs_out.at[d], rs_in.at[d], rs_i + d, (sp, xx))
        else:
            total = part
    for d in range(1, nx):
        remote(rs_in.at[d], rs_in.at[d], rs_i + d, (sp, mod(x - d, nx))).wait_recv()
        total = total + rs_in[d].astype(F32)
    out[...] = total.astype(BF16)

    for cp in pending:
        cp.wait_send()
    for ring in (wy, wz, qr, kr):
        for cp in ring.started:
            cp.wait_send()


def layer(nz, ny, nx, *args):
    (tokens, gain, wq, wk, wv, wcv, wcg, taps, cgain, cbias, cum_gate, wa, wc) = args
    dim = tokens.shape[1]
    trows = tokens.shape[0]
    rows, chip = ROWS, 2 * ROWS
    nsp = nz * ny * 2
    chans = wcv.shape[1]
    wcol = wa.shape[1]
    cols = wq.shape[1] + wk.shape[1] + wv.shape[1] + wcv.shape[1] + wcg.shape[1]
    ocols = wcol * nsp // nx
    vm = pl.BlockSpec(memory_space=pltpu.VMEM)
    hb = pl.BlockSpec(memory_space=pl.ANY)
    nsem = nx * 3 + (ny - 1) * 3 + (nz - 1) * 2 + 2 * nz + 2 * ny + 4
    scratch = [
        pltpu.VMEM((nx, trows, dim), BF16),
        pltpu.VMEM((dim, cols), BF16),
        pltpu.VMEM((rows, HEAD), BF16),
        pltpu.VMEM((ny, chip, HEAD), BF16),
        pltpu.VMEM((nz, 2, rows + HEAD, 128), BF16),
        pltpu.VMEM((32 + rows, chans), F32),
        pltpu.VMEM((32, chans), BF16),
        pltpu.VMEM((32, chans), BF16),
        pltpu.VMEM((rows, chans), F32),
        pltpu.VMEM((8, 128), F32),
        pltpu.VMEM((nx, 8, 128), F32),
        pltpu.VMEM((nz, ny, 2, wcol, 512), BF16),
        pltpu.VMEM((nz * chip, chip), F32),
        pltpu.VMEM((nz * chip, 128), F32),
        pltpu.VMEM((ny, 2, HEAD + 16, rows), BF16),
        pltpu.VMEM((ny, 2, HEAD + 16, rows), BF16),
        pltpu.VMEM((nx, rows, ocols), BF16),
        pltpu.VMEM((nx, rows, ocols), BF16),
        pltpu.VMEM((nx, rows, ocols), F32),
        pltpu.SemaphoreType.DMA((5,)),
        pltpu.SemaphoreType.DMA((nsem,)),
        pltpu.SemaphoreType.DMA((nsem,)),
    ]

    def kernel(*refs):
        layer_kernel(nz, ny, nx, *refs)

    return pl.pallas_call(
        kernel,
        out_shape=jax.ShapeDtypeStruct((rows, ocols), BF16),
        in_specs=[vm, vm, hb, hb, hb, hb, hb, vm, vm, vm, vm, vm, vm],
        out_specs=vm,
        scratch_shapes=scratch,
        compiler_params=pltpu.CompilerParams(
            collective_id=0, has_side_effects=True, vmem_limit_bytes=48 * 1024 * 1024
        ),
        name="layer",
    )(
        tokens, gain.reshape(1, dim), wq, wk, wv, wcv, wcg, taps, cgain.reshape(1, chans), cbias.reshape(1, chans),
        cum_gate.T, wa.T, wc.T,
    )


def build(mesh, nz, ny):
    nx = mesh.shape["tp"]

    def shards(*args):
        return layer(nz, ny, nx, *args)

    return jax.shard_map(
        shards,
        mesh=mesh,
        in_specs=(
            P(("sp", "tp"), None),
            P(),
            P(None, "tp"),
            P(None, "tp"),
            P(None, "tp"),
            P(None, "tp"),
            P(None, "tp"),
            P(None, "tp"),
            P("tp"),
            P("tp"),
            P(None, "tp"),
            P("tp", "sp"),
            P("tp", "sp"),
        ),
        out_specs=P("sp", "tp"),
        check_vma=False,
    )


def solution(mesh):
    side = math.isqrt(mesh.shape["sp"] // 2)
    return build(mesh, side, side)
```

```python
import math

import jax
import jax.numpy as jnp
from jax import lax
from jax.experimental import pallas as pl
from jax.experimental.pallas import tpu as pltpu
from jax.sharding import PartitionSpec as P

HEAD = 128
KW = 31
ROWS = 128
LOG2E = math.log2(math.e)
FAR = 1e30
MESH = pl.DeviceIdType.MESH
F32 = jnp.float32
BF16 = jnp.bfloat16


def nt(a, b):
    return lax.dot_general(a, b, (((1,), (1,)), ((), ())), preferred_element_type=F32)


def nn(a, b):
    return lax.dot_general(a, b, (((1,), (0,)), ((), ())), preferred_element_type=F32)


SCOPE = []


def phase(name):
    if SCOPE:
        SCOPE.pop().__exit__(None, None, None)
    if name:
        scope = jax.named_scope(name)
        scope.__enter__()
        SCOPE.append(scope)


class Sems:
    def __init__(self, send, recv):
        self.send, self.recv, self.used = send, recv, 0

    def take(self, count=1):
        first = self.used
        self.used += count
        return first


class Ring:
    def __init__(self, n, sems, plus, minus, here, there):
        self.n, self.here, self.there = n, here, there
        self.peer = {1: plus, -1: minus}
        self.hops = n // 2
        self.base = sems.take(self.hops * 4)
        self.sems = sems
        self.started = []

    def index(self, way, k, ch):
        return self.base + ((k - 1) * 2 + (way < 0)) * 2 + ch

    def rel(self, way, k):
        return k if way > 0 else (self.n - k) % self.n

    def chunks(self, way, k):
        if k < self.hops:
            return (0, 1) if way > 0 else (1, 0)
        return (0,) if way > 0 else (1,)

    def start(self, way, k, ch):
        if k > self.hops or ch not in self.chunks(way, k):
            return
        i = self.index(way, k, ch)
        a, b = self.rel(way, k - 1), self.rel(way, k)
        c = pltpu.make_async_remote_copy(
            src_ref=self.here(a, ch),
            dst_ref=self.there(a, b, ch),
            send_sem=self.sems.send.at[i],
            recv_sem=self.sems.recv.at[i],
            device_id=self.peer[way],
            device_id_type=MESH,
        )
        c.start()
        self.started.append(c)

    def begin(self, chunks=(0, 1)):
        for n in range(2):
            for way in (1, -1):
                ch = n if way > 0 else 1 - n
                if ch in chunks:
                    self.start(way, 1, ch)

    def step(self, k, after=None):
        if k > self.hops:
            return
        for n in range(2):
            for way in (1, -1):
                ch = n if way > 0 else 1 - n
                if ch not in self.chunks(way, k):
                    continue
                i = self.index(way, k, ch)
                slot = self.here(self.rel(way, k), ch)
                pltpu.make_async_remote_copy(
                    src_ref=slot,
                    dst_ref=slot,
                    send_sem=self.sems.send.at[i],
                    recv_sem=self.sems.recv.at[i],
                    device_id=self.peer[-way],
                    device_id_type=MESH,
                ).wait_recv()
                self.start(way, k + 1, ch)
                if after is not None:
                    after(self.rel(way, k), ch)


def layer_kernel(
    nz, ny, nx,
    tokens_h, gain, wq, wk, wv, wcv, wcg, taps, cgain, cbias, gate_h, wa_t, wc_t,
    out,
    tokens, gate, tok_all, wbuf, qsend, qbuf, kv, conv_in, halo_out, halo_in, conv_s, st_out, st_in,
    wta, wtc, s_ref, peak_ref, gkb, o_out, o_in, rs_out, rs_in, proj_s, wsem, send, recv,
):
    rows = ROWS
    chip = 2 * rows
    dim = tokens.shape[1]
    trows = tokens.shape[0]
    chans = wcv.shape[1]
    ocols = out.shape[1]
    sp = lax.axis_index("sp")
    x = lax.axis_index("tp")
    c = lax.rem(sp, 2)
    y = lax.rem(lax.div(sp, 2), ny)
    z = lax.div(sp, 2 * ny)
    nsp = nz * ny * 2

    def at(zz, yy, cc):
        return (zz * ny + yy) * 2 + cc

    def mod(a, n):
        return lax.rem(a + 2 * n, n)

    sems = Sems(send, recv)
    pending = []

    def remote(src, dst, i, dev, ri=None):
        return pltpu.make_async_remote_copy(
            src_ref=src,
            dst_ref=dst,
            send_sem=send.at[i],
            recv_sem=recv.at[i if ri is None else ri],
            device_id=dev,
            device_id_type=MESH,
        )

    def launch(src, dst, i, dev, ri=None):
        cp = remote(src, dst, i, dev, ri)
        cp.start()
        pending.append(cp)

    def landed(slot, i, dev):
        remote(slot, slot, i, dev).wait_recv()

    sib = (at(z, y, 1 - c), x)
    y_up, y_down = (at(z, mod(y + 1, ny), c), x), (at(z, mod(y - 1, ny), c), x)
    z_up, z_down = (at(mod(z + 1, nz), y, c), x), (at(mod(z - 1, nz), y, c), x)
    x_up, x_down = (sp, mod(x + 1, nx)), (sp, mod(x - 1, nx))
    nxt, prv = mod(sp + 1, nsp), mod(sp - 1, nsp)

    phase("load")
    first = []
    for k, (a, b) in enumerate(
        ((tokens_h, tokens), (wa_t, wta.at[z, y, c]), (wc_t, wtc.at[z, y, c]), (gate_h, gate))
    ):
        cp = pltpu.make_async_copy(a, b, wsem.at[5 + k])
        cp.start()
        first.append(cp)
    wcols, off = [], 0
    for k, w in enumerate((wq, wk, wv, wcv, wcg)):
        cp = pltpu.make_async_copy(w, wbuf.at[:, off : off + w.shape[1]], wsem.at[k])
        cp.start()
        wcols.append(cp)
        off += w.shape[1]

    barrier = pltpu.get_barrier_semaphore()
    peers = [(sp, mod(x + d, nx)) for d in range(1, nx)]
    peers += [(at(z, mod(y + d, ny), cc), x) for d in range(1, ny) for cc in range(2)]
    peers += [(at(mod(z + d, nz), y, c), x) for d in range(1, nz)]
    peers += [sib, (nxt, x), (prv, x)]
    for p in peers:
        pl.semaphore_signal(barrier, inc=1, device_id=p, device_id_type=MESH)

    first[0].wait()
    tok = tokens[...].astype(F32)
    mean_sq = jnp.mean(tok * tok, axis=-1, keepdims=True)
    tok_all[x] = (tok * lax.rsqrt(mean_sq + 1e-06) * gain[...].astype(F32).reshape(1, dim)).astype(BF16)
    first[1].wait()
    first[2].wait()

    phase("barrier")
    pl.semaphore_wait(barrier, len(peers))

    phase("send_tok")
    th = trows // 2
    tr = Ring(
        nx, sems, x_up, x_down,
        lambda r, ch: tok_all.at[mod(x - r, nx), pl.ds(ch * th, th)],
        lambda a, b, ch: tok_all.at[mod(x - a, nx), pl.ds(ch * th, th)],
    )
    tr.begin()

    w1_i = sems.take(ny + nz)
    for d in sorted(range(1, ny), key=lambda d: -min(d, ny - d)):
        launch(wta.at[z, y, c], wta.at[z, y, c], w1_i + d, (at(z, mod(y + d, ny), c), x))
    for d in sorted(range(1, nz), key=lambda d: -min(d, nz - d)):
        launch(wtc.at[z, y, c], wtc.at[z, y, c], w1_i + ny + d, (at(mod(z + d, nz), y, c), x))
    yh, zh = ny // 2, nz // 2
    war = Ring(
        nz, sems, z_up, z_down,
        lambda r, ch: wta.at[mod(z - r, nz), pl.ds(ch * yh, yh), c],
        lambda a, b, ch: wta.at[mod(z - a, nz), pl.ds(ch * yh, yh), c],
    )
    wcr = Ring(
        ny, sems, y_up, y_down,
        lambda r, ch: wtc.at[pl.ds(ch * zh, zh), mod(y - r, ny), c],
        lambda a, b, ch: wtc.at[pl.ds(ch * zh, zh), mod(y - a, ny), c],
    )
    was_i, wcs_i = sems.take(2 * nz), sems.take(2 * ny)

    def pass_wa(rel, ch):
        slot = war.here(rel, ch)
        launch(slot, slot, was_i + 2 * rel + ch, sib)

    def pass_wc(rel, ch):
        slot = wcr.here(rel, ch)
        launch(slot, slot, wcs_i + 2 * rel + ch, sib)

    def w_step(k):
        war.step(k, pass_wa)
        wcr.step(k, pass_wc)

    def core_rows(ch):
        return pl.ds(pl.multiple_of((c if ch == 0 else 1 - c) * rows, rows), rows)

    qr = Ring(
        ny, sems, y_up, y_down,
        lambda r, ch: qbuf.at[r, core_rows(ch)],
        lambda a, b, ch: qbuf.at[b, core_rows(ch)],
    )
    kr = Ring(
        nz, sems, z_up, z_down,
        lambda r, ch: kv.at[r, 0, pl.ds(ch * rows, rows)],
        lambda a, b, ch: kv.at[b, 0, pl.ds(ch * rows, rows)],
    )
    ks_i = sems.take(2 * nz)

    def pass_kv(rel, ch):
        part = pl.ds(ch * rows, rows)
        launch(kv.at[rel, 0, part], kv.at[rel, 1, part], ks_i + 2 * rel + ch, sib)

    def wait_kv(rel, ch):
        landed(kv.at[rel, 1, pl.ds(ch * rows, rows)], ks_i + 2 * rel + ch, sib)

    phase("gates")
    first[3].wait()
    g_first = gate[:, pl.ds(pl.multiple_of(z * ny * chip, chip), 128)]
    g_ref = jnp.where(c == 0, g_first[0:1, 0:1], g_first[1:2, 0:1])

    def gate_row(start, width):
        g = gate[:, pl.ds(pl.multiple_of(start, 128), width)]
        return (jnp.where(c == 0, g[0:1], g[1:2]) - g_ref) * LOG2E

    for s in range(nz):
        for p in range(2):
            cc = c if p == 0 else 1 - c
            g = gate_row(at(mod(z - s, nz), y, cc) * rows, rows)
            g = jnp.where(s <= z, g, FAR)
            gkb[pl.ds((s * 2 + p) * rows, rows), :] = jnp.transpose(jnp.broadcast_to(g, (128, rows)))
    for r in range(ny):
        peak_ref[r] = jnp.full((8, chip), -FAR, F32)

    phase("tok1")
    tr.step(1)
    phase("w1")
    for d in range(1, ny):
        yy = mod(y - d, ny)
        landed(wta.at[z, yy, c], w1_i + d, (at(z, yy, c), x))
    for d in range(1, nz):
        zz = mod(z - d, nz)
        landed(wtc.at[zz, y, c], w1_i + ny + d, (at(zz, y, c), x))
    war.begin()
    wcr.begin()
    phase("wait_w")
    for cp in wcols[:3]:
        cp.wait()
    phase("tok2")
    for k in range(2, nx // 2 + 1):
        tr.step(k)

    phase("qkv")
    normed = tok_all[...].reshape(rows, dim)
    qw, kw_ = wq.shape[1], wk.shape[1]
    qkv = nn(normed, wbuf[:, : qw + 2 * kw_])
    q0 = qkv[:, :HEAD].astype(BF16)
    q1 = qkv[:, HEAD:qw].astype(BF16)
    kv[0, 0, :rows] = qkv[:, qw : qw + kw_].astype(BF16)
    kv[0, 0, rows:] = jnp.transpose(qkv[:, qw + kw_ :]).astype(BF16)
    mine = core_rows(0)
    qbuf[0, mine] = jnp.where(c == 0, q0, q1)
    qsend[...] = jnp.where(c == 0, q1, q0)

    q_i = sems.take()
    launch(qsend, qbuf.at[0, mine], q_i, sib)
    kr.begin()
    qr.begin((0,))
    for ch in range(2):
        pass_kv(0, ch)

    phase("glu")
    for cp in wcols[3:]:
        cp.wait()
    halves = nn(normed, wbuf[:, qw + 2 * kw_ :])
    phase("wait_qsib")
    landed(qbuf.at[0, core_rows(1)], q_i, sib)
    qr.begin((1,))
    phase("glu2")
    glu = (halves[:, :chans] * jax.nn.sigmoid(halves[:, chans:])).astype(BF16)
    conv_in[32:] = glu.astype(F32)
    halo_out[...] = glu[rows - 32 :]
    h_i = sems.take()
    launch(halo_out, halo_in, h_i, (nxt, x))
    for ch in range(2):
        for rel in range(1):
            pass_wa(rel, ch)
            pass_wc(rel, ch)

    scale = LOG2E / math.sqrt(HEAD)
    key_lo = lax.broadcasted_iota(jnp.int32, (rows, chip), 0)
    q_at = lax.broadcasted_iota(jnp.int32, (rows, chip), 1)
    done = set()

    def logits(q_slots, k_slots):
        for r in q_slots:
            parts = [(s, p) for s, p in k_slots if (r, s, p) not in done]
            done.update((r, s, p) for s, p in parts)
            if not parts:
                continue
            all_t = nt(jnp.concatenate([kv[s, p, :rows] for s, p in parts], axis=0), qbuf[r])
            peak = peak_ref[r]
            for n, (s, p) in enumerate(parts):
                own = pl.ds((s * 2 + p) * rows, rows)
                g = gkb[own, :]
                t = all_t[n * rows : (n + 1) * rows] * scale - jnp.concatenate([g, g], axis=1)
                if s == 0:
                    cc = c if p == 0 else 1 - c
                    shift = (y - mod(y - r, ny)) * chip + cc * rows
                    t = jnp.where(key_lo + shift <= q_at, t, -FAR)
                s_ref[r, own, :] = t
                peak = jnp.maximum(peak, jnp.max(t.reshape(rows // 8, 8, chip), axis=0))
            peak_ref[r] = peak

    def near(n, k):
        return sorted({d % n for d in range(-min(k, n // 2), min(k, n // 2) + 1)})

    got = set()

    def hop(k):
        qr.step(k)
        kr.step(k, pass_kv)

    def catch_up(k):
        own = [(s, 0) for s in near(nz, k)]
        for s in near(nz, k - 1):
            if s not in got:
                wait_kv(s, 0)
                got.add(s)
        logits(near(ny, k), own + [(s, 1) for s in sorted(got)])

    phase("hop1")
    hop(1)
    phase("w_hop1")
    w_step(1)
    phase("conv_in")
    landed(halo_in, h_i, (prv, x))
    conv_in[:32] = jnp.where(sp == 0, 0.0, halo_in[...].astype(F32))
    tap = taps[...].astype(F32)
    half = KW // 2
    conv = jnp.zeros((rows, chans), F32)
    for k in range(half):
        conv = conv + tap[k : k + 1] * conv_in[2 + k : 2 + k + rows]
    conv_s[...] = conv
    phase("logits1")
    catch_up(1)
    phase("hop2")
    hop(2)
    phase("conv2")
    conv = conv_s[...]
    for k in range(half, KW):
        conv = conv + tap[k : k + 1] * conv_in[2 + k : 2 + k + rows]
    conv_s[...] = conv
    s1 = jnp.sum(conv, axis=1, keepdims=True)
    s2 = jnp.sum(conv * conv, axis=1, keepdims=True)
    lane = lax.broadcasted_iota(jnp.int32, (rows, 128), 1)
    st_out[...] = jnp.transpose(jnp.where(lane == 0, s1, s2))[:8]
    st_i = sems.take(nx)
    for d in range(1, nx):
        launch(st_out, st_in.at[nx - d], st_i + d, (sp, mod(x + d, nx)))
    phase("logits2")
    catch_up(2)
    phase("hop3")
    hop(3)
    phase("logits3")
    catch_up(3)
    phase("hop4")
    for k in range(4, max(ny, nz) // 2 + 1):
        hop(k)
    phase("w_hop2")
    w_step(2)
    phase("logits4")
    catch_up(max(ny, nz) // 2)
    phase("wait_kvsib")
    catch_up(max(ny, nz) // 2 + 1)
    for s in range(nz):
        wait_kv(s, 1)

    ones = jnp.ones((16, chip), BF16)
    o_i = sems.take(ny * 2)
    sub = lax.broadcasted_iota(jnp.int32, (16, rows), 0)

    def attend(r):
        jq = mod(y - r, ny)
        m = jnp.max(peak_ref[r], axis=0, keepdims=True)
        acc = jnp.zeros((HEAD + 16, chip), F32)
        for s in range(nz):
            w = jnp.exp2(s_ref[r, pl.ds(s * chip, chip), :] - m).astype(BF16)
            vt = jnp.concatenate([kv[s, 0, rows:], kv[s, 1, rows:]], axis=1)
            acc = acc + nn(jnp.concatenate([vt, ones], axis=0), w)
        den = acc[HEAD : HEAD + 1]
        o = (acc[:HEAD] / den).astype(BF16)
        m = m + gate_row((z * ny + jq) * chip, chip)
        m1 = m.astype(BF16).astype(F32)
        m2 = (m - m1).astype(BF16).astype(F32)
        d1 = den.astype(BF16).astype(F32)
        d2 = (den - d1).astype(BF16).astype(F32)
        parts = (m1, m2, m - m1 - m2, d1, d2, den - d1 - d2)
        for cc in range(2):
            lanes = slice(cc * rows, (cc + 1) * rows)
            tile = jnp.zeros((16, rows), F32)
            for i, part in enumerate(parts):
                tile = jnp.where(sub == i, part[:, lanes], tile)
            o_out[r, cc, :HEAD] = o[:, lanes]
            o_out[r, cc, HEAD:] = tile.astype(BF16)

    ring_order = sorted(range(ny), key=lambda r: (-min(r, ny - r), r))
    for n, r in enumerate(ring_order):
        phase(f"attend{n}")
        attend(r)
        phase(f"sendo{n}")
        if r:
            for cc in range(2):
                launch(
                    o_out.at[r, cc], o_in.at[r, c], o_i + 2 * r + cc, (at(z, mod(y - r, ny), cc), x), o_i + 2 * r + c
                )
        if n == ny // 2 - 1:
            w_step(3)
    launch(o_out.at[0, 1 - c], o_in.at[0, c], o_i + 1 - c, sib, o_i + c)

    phase("chan_norm")
    tot = st_out[...]
    for d in range(1, nx):
        landed(st_in.at[nx - d], st_i + d, (sp, mod(x - d, nx)))
        tot = tot + st_in[nx - d]
    total_chans = chans * nx
    mean_r = tot[0:1] / total_chans
    var_r = tot[1:2] / total_chans - mean_r * mean_r
    rstd_r = lax.rsqrt(var_r + 1e-05)
    mean_c = jnp.transpose(jnp.broadcast_to(mean_r, (128, rows)))
    rstd_c = jnp.transpose(jnp.broadcast_to(rstd_r, (128, rows)))
    wide = chans // 128
    mean_c = jnp.concatenate([mean_c] * wide, axis=1)
    rstd_c = jnp.concatenate([rstd_c] * wide, axis=1)
    shaped = (conv_s[...] - mean_c) * rstd_c * cgain[...].astype(F32).reshape(1, chans)
    shaped = shaped + cbias[...].astype(F32).reshape(1, chans)
    conv_act = (shaped / (1.0 + jnp.exp(-shaped))).astype(BF16)

    phase("w_hop4")
    for k in range(4, max(ny, nz) // 2 + 1):
        w_step(k)
    phase("wait_wsib")
    for s in range(nz):
        for ch in range(2):
            slot = wta.at[mod(z - s, nz), pl.ds(ch * yh, yh), 1 - c]
            landed(slot, was_i + 2 * s + ch, sib)
    for s in range(ny):
        for ch in range(2):
            slot = wtc.at[pl.ds(ch * zh, zh), mod(y - s, ny), 1 - c]
            landed(slot, wcs_i + 2 * s + ch, sib)
    phase("proj_conv")
    per = nz // nx
    for d in range(nx):
        xx = mod(x + d, nx)
        w = wtc[pl.ds(xx * per, per)].reshape(ocols, chans)
        proj_s[d] = nt(conv_act, w)

    phase("wait_o")
    o_in[0, c] = o_out[0, c]
    for r in range(1, ny):
        for hh in range(2):
            landed(o_in.at[r, hh], o_i + 2 * r + hh, (at(z, mod(y + r, ny), hh), x))
    landed(o_in.at[0, 1 - c], o_i + 1 - c, sib)
    phase("merge")
    heads = []
    for hh in range(2):
        tiles = [o_in[r, hh, HEAD:].astype(F32) for r in range(ny)]
        tops = [t[0:1] + t[1:2] + t[2:3] for t in tiles]
        dens = [t[3:4] + t[4:5] + t[5:6] for t in tiles]
        top = tops[0]
        for t in tops[1:]:
            top = jnp.maximum(top, t)
        scaled = [d * jnp.exp2(t - top) for d, t in zip(dens, tops)]
        den = scaled[0]
        for d in scaled[1:]:
            den = den + d
        acc = jnp.zeros((HEAD, rows), F32)
        for r in range(ny):
            acc = acc + o_in[r, hh, :HEAD].astype(F32) * (scaled[r] / den)
        heads.append(jnp.transpose(acc).astype(BF16))
    attended = jnp.concatenate(heads, axis=1)

    phase("proj_att")
    rs_i = sems.take(nx)
    for d in sorted(range(1, nx), key=lambda d: -min(d, nx - d)) + [0]:
        xx = mod(x + d, nx)
        w = wta[pl.ds(xx * per, per)].reshape(ocols, wta.shape[4])
        part = proj_s[d] + nt(attended, w)
        if d:
            rs_out[d] = part.astype(BF16)
            launch(rs_out.at[d], rs_in.at[d], rs_i + d, (sp, xx))
        else:
            total = part
    phase("wait_rs")
    for d in range(1, nx):
        landed(rs_in.at[d], rs_i + d, (sp, mod(x - d, nx)))
        total = total + rs_in[d].astype(F32)
    out[...] = total.astype(BF16)

    phase("wait_send")
    for cp in pending:
        cp.wait_send()
    for ring in (tr, war, wcr, qr, kr):
        for cp in ring.started:
            cp.wait_send()
    phase(None)


def layer(nz, ny, nx, *args):
    (tokens, gain, wq, wk, wv, wcv, wcg, taps, cgain, cbias, cum_gate, wa, wc) = args
    dim = tokens.shape[1]
    trows = tokens.shape[0]
    rows, chip = ROWS, 2 * ROWS
    nsp = nz * ny * 2
    chans = wcv.shape[1]
    wcol = wa.shape[1]
    cols = wq.shape[1] + wk.shape[1] + wv.shape[1] + wcv.shape[1] + wcg.shape[1]
    ocols = wcol * nsp // nx
    vm = pl.BlockSpec(memory_space=pltpu.VMEM)
    hb = pl.BlockSpec(memory_space=pltpu.HBM)
    nsem = 4 * nx + 9 * ny + 9 * nz + 2
    scratch = [
        pltpu.VMEM((trows, dim), BF16),
        pltpu.VMEM((2, nsp * rows), F32),
        pltpu.VMEM((nx, trows, dim), BF16),
        pltpu.VMEM((dim, cols), BF16),
        pltpu.VMEM((rows, HEAD), BF16),
        pltpu.VMEM((ny, chip, HEAD), BF16),
        pltpu.VMEM((nz, 2, rows + HEAD, 128), BF16),
        pltpu.VMEM((32 + rows, chans), F32),
        pltpu.VMEM((32, chans), BF16),
        pltpu.VMEM((32, chans), BF16),
        pltpu.VMEM((rows, chans), F32),
        pltpu.VMEM((8, 128), F32),
        pltpu.VMEM((nx, 8, 128), F32),
        pltpu.VMEM((nz, ny, 2, wcol, 256), BF16),
        pltpu.VMEM((nz, ny, 2, wcol, 256), BF16),
        pltpu.VMEM((ny, nz * chip, chip), F32),
        pltpu.VMEM((ny, 8, chip), F32),
        pltpu.VMEM((nz * chip, 128), F32),
        pltpu.VMEM((ny, 2, HEAD + 16, rows), BF16),
        pltpu.VMEM((ny, 2, HEAD + 16, rows), BF16),
        pltpu.VMEM((nx, rows, ocols), BF16),
        pltpu.VMEM((nx, rows, ocols), BF16),
        pltpu.VMEM((nx, rows, ocols), F32),
        pltpu.SemaphoreType.DMA((9,)),
        pltpu.SemaphoreType.DMA((nsem,)),
        pltpu.SemaphoreType.DMA((nsem,)),
    ]

    def kernel(*refs):
        layer_kernel(nz, ny, nx, *refs)

    return pl.pallas_call(
        kernel,
        out_shape=jax.ShapeDtypeStruct((rows, ocols), BF16),
        in_specs=[hb, vm, hb, hb, hb, hb, hb, vm, vm, vm, hb, hb, hb],
        out_specs=vm,
        scratch_shapes=scratch,
        compiler_params=pltpu.CompilerParams(
            collective_id=0, has_side_effects=True, vmem_limit_bytes=60 * 1024 * 1024
        ),
        name="layer",
    )(
        tokens, gain, wq, wk, wv, wcv, wcg, taps, cgain, cbias, cum_gate.T, wa.T, wc.T
    )


def build(mesh, nz, ny):
    nx = mesh.shape["tp"]

    def shards(*args):
        return layer(nz, ny, nx, *args)

    return jax.shard_map(
        shards,
        mesh=mesh,
        in_specs=(
            P(("sp", "tp"), None),
            P(),
            P(None, "tp"),
            P(None, "tp"),
            P(None, "tp"),
            P(None, "tp"),
            P(None, "tp"),
            P(None, "tp"),
            P("tp"),
            P("tp"),
            P(None, "tp"),
            P("tp", "sp"),
            P("tp", "sp"),
        ),
        out_specs=P("sp", "tp"),
        check_vma=False,
    )


def solution(mesh):
    side = math.isqrt(mesh.shape["sp"] // 2)
    return build(mesh, side, side)
```
